512 devices in a mesh: sp: 32 (over z, core), tp: 16 (over y, x).
Axes of the slice: x: 4, y: 4, z: 16, core: 2. Of those that a mesh axis runs over, the one named last changes fastest.
Arguments:
- moe_input: bfloat16 [4096, 2048], P('sp', 'tp'), may hold values from -6 to 6
- cotangent: bfloat16 [4096, 2048], P('sp', 'tp'), may hold values from -6 to 6
- routes: int32 [4096, 2], P('sp'), may hold values from 0 to 31, all different within a row; in each aligned block of 128 rows (0 to 127, 128 to 255, ...) at most 16 rows name the same one
- route_weight: float32 [4096, 2], P('sp'), may hold values from 0.1 to 1
- w_gate: bfloat16 [32, 2816, 2048], P('sp', 'tp'), may hold values from -0.125 to 0.125
- w_up: bfloat16 [32, 2816, 2048], P('sp', 'tp'), may hold values from -0.125 to 0.125
- w_down: bfloat16 [32, 2816, 2048], P('sp', 'tp'), may hold values from -0.109375 to 0.109375
- v_value: bfloat16 [4096, 1024], P('sp', 'tp'), may hold values from -6 to 6
- v_gate: bfloat16 [4096, 1024], P('sp', 'tp'), may hold values from -12 to 12
- conv_out: bfloat16 [4096, 1024], P('sp', 'tp'), may hold values from -6 to 6
- row_mean: float32 [4096], P('sp'), may hold values from -3 to 3
- row_rstd: float32 [4096], P('sp'), may hold values from 0.5 to 2
- ln_gain: float32 [1024], P('tp'), may hold values from 0.1 to 1.9
- taps: bfloat16 [31, 1024], P(None, 'tp'), may hold values from -1 to 1
- out_proj: bfloat16 [2048, 1024], P('sp', 'tp'), may hold values from -0.1875 to 0.1875
Outputs:
- gate_grad: bfloat16 [32, 2816, 2048], P('sp', 'tp')
- up_grad: bfloat16 [32, 2816, 2048], P('sp', 'tp')
- down_grad: bfloat16 [32, 2816, 2048], P('sp', 'tp')
- proj_grad: float32 [2048, 1024], P('sp', 'tp')
- stream_grad: bfloat16 [4096, 2048], P('sp', 'tp')
- value_grad: bfloat16 [4096, 1024], P('sp', 'tp')
- gating_grad: bfloat16 [4096, 1024], P('sp', 'tp')
The draws below stay inside these ranges and needn't reach their ends.
Inputs may be any that keep to these rules, and one draw needn't show every extreme that they name: `routes`: in the rows of one device no expert is named more than 16 times.
All inputs are finite; a program needn't handle non-finite values.
Results may differ from the reference program's by a relative error of at most 0.025.
Values may be sent and summed in bfloat16 or wider, within the bound.
A program may use at most 64 MiB of HBM per device.

```python
import math
import jax
import jax.numpy as jnp
import numpy as np
from jax import lax

D = 2048
FF = 2816
CW = 1024
KERNEL = 31
TOK_DEV = 128
TOKENS = 4096
EXPERTS = 32
CAP = 16
N_SP = 32
N_TP = 16


def spiked(values, key, source, target, shards_of, factor):
    def block_of(axis_at):
        return (jnp.arange(values.shape[axis_at]) // (values.shape[axis_at] // shards_of)).reshape((-1,) + (1,) * (values.ndim - 1 - axis_at))

    first = jax.random.permutation(key, shards_of)[block_of(target)]
    other_side = (block_of(target) + shards_of // 2) % shards_of
    return jnp.where((block_of(source) == first) | (block_of(source) == other_side), factor * values, values)


def shard_levels(rng, extent, split, least, top_value):
    loudness = 1.0
    for dim, shards_of in split:
        draws = jax.random.uniform(jax.random.fold_in(jax.random.fold_in(rng, 6), dim), (shards_of,), jnp.float32, least / len(split), top_value / len(split))
        loudness = loudness * jnp.repeat(jnp.exp(draws), extent[dim] // shards_of).reshape((-1,) + (1,) * (len(extent) - 1 - dim))
    return loudness


def routed_block(rng, own, number, rows, number_of, top, bound, lean):
    sequence = jax.random.permutation(rng, number_of)
    crowded, usual = portions_of(number_of, rows * top, bound, lean, True), portions_of(number_of, rows * top, bound, lean, False)
    places = jnp.arange(number_of)

    def named(sizes, offset_by):
        used = int((sizes > 0).sum())
        fixed = max(1, used // 4)
        passed = fixed + (places - fixed + offset_by * (used - fixed)) % max(1, number_of - fixed)
        return jnp.zeros((number_of,), jnp.int32).at[sequence[jnp.where(places < fixed, places, passed)]].set(jnp.asarray(sizes, jnp.int32))

    sizes = jnp.where(number % 4 == 0, named(crowded, number // 4), named(usual, number - number // 4 - 1))
    mixed = jax.random.permutation(jax.random.fold_in(own, 3), number_of)
    source_of, receiver = mixed[0:number_of // 2 * 2:2], mixed[1:number_of // 2 * 2:2]
    slack = jnp.minimum(sizes[source_of] - 1, bound - sizes[receiver]) // 2
    slack = jnp.where((source_of == sequence[0]) | (receiver == sequence[0]) | (sizes[receiver] == 0), 0, jnp.maximum(slack, 0))
    passed = jax.random.randint(jax.random.fold_in(own, 4), (number_of // 2,), 0, 1 << 20) % (slack + 1)
    sizes = sizes.at[source_of].add(-passed).at[receiver].add(passed)
    members = jnp.searchsorted(jnp.cumsum(sizes), jnp.arange(rows * top), side="right").astype(jnp.int32)
    table = members.reshape(top, rows).T
    table = table[jax.random.permutation(jax.random.fold_in(own, 1), rows)]
    offset_by = jax.random.randint(jax.random.fold_in(own, 2), (rows, 1), 0, top)
    return jnp.take_along_axis(table, (jnp.arange(top)[None, :] + offset_by) % top, axis=1)


def portions_of(number_of, total, reach, lean, full):
    portions = [(1 << 20) // math.isqrt(standing ** lean) + 1 for standing in range(1, number_of + 1)]
    largest = reach if full else min(reach, max(-(-total // number_of), total * portions[0] // sum(portions)))
    least = 1 if total - largest >= number_of - 1 else 0
    holding, rest = [largest] + [least] * (number_of - 1), total - largest - least * (number_of - 1)
    while rest > 0:
        movable = [i for i in range(1, number_of) if holding[i] < largest] or [i for i in range(1, number_of) if holding[i] < reach]
        pool, budget = sum([portions[i] for i in movable]), rest
        for i in movable:
            addition = min(reach - holding[i], max(1, budget * portions[i] // pool), rest)
            holding[i] = holding[i] + addition
            rest = rest - addition
    return np.array(holding)


def scatter_about(rng, shape, deviation, reach, shards=(), kind=jnp.bfloat16):
    array = jax.random.normal(rng, shape, jnp.float32) * deviation
    if len(shards) > 0:
        array = shard_levels(rng, shape, shards, -0.22, 0.18) * array
    return jnp.clip(array, min=-reach, max=reach).astype(kind)


def heavy_noise(stream_key, dims, deviation, most, shards, heavy, kind=jnp.bfloat16):
    values = deviation * jax.random.normal(stream_key, dims, jnp.float32)
    if shards:
        values = values * shard_levels(stream_key, dims, shards, -0.22, 0.18)
    return jnp.clip(spiked(values, jax.random.fold_in(stream_key, 3), *heavy), -most, most).astype(kind)


def setup_inputs(seed: int = 0) -> dict:
    key_list = jax.random.split(jax.random.key(seed), 16)
    moe_input = scatter_about(key_list[0], (TOKENS, D), 1.0, 6.0, ((0, 32), (1, 16)))
    cotangent = heavy_noise(key_list[1], (TOKENS, D), 1.0, 6.0, ((0, 32), (1, 16)), (0, 1, 32, 2.75))
    routes_keys = jax.random.split(jax.random.fold_in(key_list[2], 1), TOKENS // TOK_DEV)
    routes_turns = jax.random.permutation(jax.random.fold_in(key_list[2], 3), TOKENS // TOK_DEV)
    routes = jax.vmap(lambda own, number: routed_block(jax.random.fold_in(key_list[2], 2), own, number, TOK_DEV, EXPERTS, 2, CAP, 2))(routes_keys, routes_turns).reshape((TOKENS, 2))
    route_weight = jnp.clip(0.1 + 0.9 * jax.random.uniform(key_list[3], (TOKENS, 2), jnp.float32) ** shard_levels(key_list[3], (TOKENS, 2), ((0, 32),), -0.2, 0.2), 0.1, 1.0)
    w_gate = scatter_about(key_list[4], (EXPERTS, FF, D), D ** -0.5, 0.125, ((0, 32), (1, 16)))
    w_up = scatter_about(key_list[5], (EXPERTS, FF, D), D ** -0.5, 0.125, ((0, 32), (1, 16)))
    w_down = scatter_about(key_list[6], (EXPERTS, FF, D), FF ** -0.5, 0.109375, ((0, 32), (1, 16)))
    v_value = scatter_about(key_list[7], (TOKENS, CW), 1.0, 6.0, ((0, 32), (1, 16)))
    v_gate = scatter_about(key_list[8], (TOKENS, CW), 2.0, 12.0, ((0, 32), (1, 16)))
    conv_out = scatter_about(key_list[9], (TOKENS, CW), 1.0, 6.0, ((0, 32), (1, 16)))
    row_mean = scatter_about(key_list[10], (TOKENS,), 0.5, 3.0, ((0, 32),), jnp.float32)
    row_rstd = jnp.clip(jnp.exp(math.log(2.0) - 1.3862944 * jax.random.uniform(key_list[11], (TOKENS,), jnp.float32) ** shard_levels(key_list[11], (TOKENS,), ((0, 32),), -0.2, 0.2)), 0.5, 2.0)
    ln_gain = jnp.clip(1.0 + 0.18 * jax.random.normal(key_list[12], (CW,), jnp.float32), 0.1, 1.9)
    taps = scatter_about(key_list[13], (KERNEL, CW), KERNEL ** -0.5, 1.0, ((1, 16),))
    out_proj = scatter_about(key_list[14], (D, CW), CW ** -0.5, 0.1875, ((0, 32), (1, 16)))
    return {"moe_input": moe_input, "cotangent": cotangent, "routes": routes, "route_weight": route_weight, "w_gate": w_gate, "w_up": w_up, "w_down": w_down, "v_value": v_value, "v_gate": v_gate, "conv_out": conv_out, "row_mean": row_mean, "row_rstd": row_rstd, "ln_gain": ln_gain, "taps": taps, "out_proj": out_proj}


def slot_numbers(block_routes):
    member = (block_routes[:, None] == jnp.arange(N_SP, dtype=jnp.int32)[None, :]).astype(jnp.int32)
    earlier = jnp.cumsum(member, axis=0) - member
    return jnp.sum(earlier * member, axis=1).astype(jnp.int32)


def expert_pass(operands):
    rows, cotan, gate_w, up_w, down_w = operands
    total = rows.shape[0]
    gate_pre = jnp.dot(rows, gate_w.T, preferred_element_type=jnp.float32)
    up_pre = jnp.dot(rows, up_w.T, preferred_element_type=jnp.float32)
    gate_sig = jax.nn.sigmoid(gate_pre)
    gate_act = gate_pre * gate_sig
    hidden = (gate_act * up_pre).astype(jnp.bfloat16)
    down_g = jnp.dot(hidden.T, cotan, preferred_element_type=jnp.float32).astype(jnp.bfloat16)
    hidden_grad = jnp.dot(cotan, down_w.T, preferred_element_type=jnp.float32)
    gate_delta = (hidden_grad * up_pre * gate_sig * (1.0 + gate_pre * (1.0 - gate_sig))).astype(jnp.bfloat16)
    up_delta = (hidden_grad * gate_act).astype(jnp.bfloat16)
    gate_g = jnp.dot(gate_delta.T, rows, preferred_element_type=jnp.float32).astype(jnp.bfloat16)
    up_g = jnp.dot(up_delta.T, rows, preferred_element_type=jnp.float32).astype(jnp.bfloat16)
    per_block = FF // N_TP
    gate_three = gate_delta.astype(jnp.float32).reshape(total, N_TP, per_block)
    up_three = up_delta.astype(jnp.float32).reshape(total, N_TP, per_block)
    gate_wt = gate_w.astype(jnp.float32).reshape(N_TP, per_block, D)
    up_wt = up_w.astype(jnp.float32).reshape(N_TP, per_block, D)
    partial_value = jnp.einsum('rnf,nfd->nrd', gate_three, gate_wt) + jnp.einsum('rnf,nfd->nrd', up_three, up_wt)
    rounded = lax.optimization_barrier(partial_value.astype(jnp.bfloat16))
    row_g = jnp.sum(rounded.astype(jnp.float32), axis=0).astype(jnp.bfloat16)
    return gate_g, up_g, down_g, row_g


def reference(moe_input, cotangent, routes, route_weight, w_gate, w_up, w_down, v_value, v_gate,
              conv_out, row_mean, row_rstd, ln_gain, taps, out_proj):
    buffer_len = N_SP * CAP
    block_routes = routes.reshape(N_SP, 2 * TOK_DEV).astype(jnp.int32)
    slot_index = jax.vmap(slot_numbers)(block_routes)
    source = jnp.arange(N_SP, dtype=jnp.int32)[:, None]
    buffer_row = (block_routes * buffer_len + source * CAP + slot_index).reshape(-1).astype(jnp.int32)
    token_index = (jnp.arange(2 * TOKENS, dtype=jnp.int32) // 2).astype(jnp.int32)
    picked = moe_input[token_index]
    weighted = (route_weight.reshape(-1)[:, None] * cotangent[token_index].astype(jnp.float32)).astype(jnp.bfloat16)
    rows_all = jnp.zeros((EXPERTS * buffer_len, D), jnp.bfloat16).at[buffer_row].set(picked)
    cotan_all = jnp.zeros((EXPERTS * buffer_len, D), jnp.bfloat16).at[buffer_row].set(weighted)
    rows_all = rows_all.reshape(EXPERTS, buffer_len, D)
    cotan_all = cotan_all.reshape(EXPERTS, buffer_len, D)
    gate_g, up_g, down_g, row_g = lax.map(expert_pass, (rows_all, cotan_all, w_gate, w_up, w_down))
    returned = row_g.reshape(EXPERTS * buffer_len, D)[buffer_row].astype(jnp.float32)
    returned = returned.reshape(TOKENS, 2, D)
    stream = cotangent.astype(jnp.float32) + (returned[:, 0] + returned[:, 1])
    stream = stream.astype(jnp.bfloat16)
    normed = (conv_out.astype(jnp.float32) - row_mean[:, None]) * row_rstd[:, None]
    scaled_norm = normed * ln_gain[None, :]
    norm_sig = jax.nn.sigmoid(scaled_norm)
    mixed = (scaled_norm * norm_sig).astype(jnp.bfloat16)
    mixed_grad = jnp.dot(stream, out_proj, preferred_element_type=jnp.float32)
    proj_g = jnp.dot(stream.T, mixed, preferred_element_type=jnp.float32)
    norm_grad = mixed_grad * norm_sig * (1.0 + scaled_norm * (1.0 - norm_sig)) * ln_gain[None, :]
    first_mean = jnp.mean(norm_grad, axis=1, keepdims=True)
    second_mean = jnp.mean(norm_grad * normed, axis=1, keepdims=True)
    conv_grad = row_rstd[:, None] * (norm_grad - first_mean - normed * second_mean)
    extended = jnp.concatenate([conv_grad, jnp.zeros((KERNEL - 1, CW), jnp.float32)], axis=0)
    tap_values = taps.astype(jnp.float32)
    unit_grad = jnp.zeros((TOKENS, CW), jnp.float32)
    for offset in range(KERNEL):
        lead = KERNEL - 1 - offset
        unit_grad = unit_grad + tap_values[offset][None, :] * extended[lead:lead + TOKENS]
    gate_sig = jax.nn.sigmoid(v_gate.astype(jnp.float32))
    value_g = (unit_grad * gate_sig).astype(jnp.bfloat16)
    gating_g = (unit_grad * v_value.astype(jnp.float32) * gate_sig * (1.0 - gate_sig)).astype(jnp.bfloat16)
    return (gate_g, up_g, down_g, proj_g, stream, value_g, gating_g)
```

```python
import jax
import jax.numpy as jnp
from jax import lax
from jax.experimental import pallas as pl
from jax.experimental.pallas import tpu as pltpu
from jax.sharding import PartitionSpec as P

MESH = pl.DeviceIdType.MESH
F32 = jnp.float32
BF16 = jnp.bfloat16
ORDER = (0, 1, 15, 2, 14, 3, 13, 4, 12, 5, 11, 6, 10, 7, 9, 8)
PLACE = {r: i for i, r in enumerate(ORDER)}
G = 4
K = 8
HK = 4
QK = 2
FO = (0, 3, 1, 2)


def dot(a, b, ca, cb):
    return lax.dot_general(a, b, (((ca,), (cb,)), ((), ())), preferred_element_type=F32)


def iota(shape, dim):
    return lax.broadcasted_iota(jnp.int32, shape, dim)


def columns_of(row):
    return jnp.transpose(jnp.broadcast_to(row, (128, 128)))


def kernel(
    routes_ref, weight_ref, mi_ref, cot_ref, wg_ref, wu_ref, wd_ref, vv_ref, vg_ref, co_ref,
    mean_ref, rstd_ref, gain_ref, taps_ref, op_ref,
    gate_out, up_out, down_out, proj_out, stream_out, value_out, gating_out,
    S, X, W, GO, PB, T1, T2, Q, V, FN, RT, FS, DT, PT, OB, OPT, TT, TB, NM, FC, MX,
    GP, GI, GS, GR, SB, SR, CG, HB,
    w_sem, o_sem, sA, rA, sB, b1, b1f, b2, b2f, s1, r1, r2, s3, r3, sR, rR, sF, rF,
    sO, rO, sD, rD, sG, rG, sS, rS, sH, rH,
):
    sp, tp = lax.axis_index("sp"), lax.axis_index("tp")
    z, c = sp // 2, sp % 2
    y, x = tp // 4, tp % 4
    partner = z * 2 + 1 - c

    def J(h, fo, so):
        yy, xx = (so, fo) if h == 0 else (fo, so)
        return ((y + yy) % 4) * 4 + (x + xx) % 4

    def chip(d, core):
        return ((z + d) % 16) * 2 + core

    def send(src, dst, ssem, rsem, dev):
        pltpu.make_async_remote_copy(
            src_ref=src, dst_ref=dst, send_sem=ssem, recv_sem=rsem, device_id=dev, device_id_type=MESH
        ).start()

    def wait(ref, sem):
        pltpu.make_async_copy(ref, ref, sem).wait()

    barrier = pltpu.get_barrier_semaphore()
    for d in range(16):
        for core in range(2):
            if d == 0:
                continue
            pl.semaphore_signal(barrier, inc=1, device_id=(chip(d, core), tp), device_id_type=MESH)
    pl.semaphore_signal(barrier, inc=1, device_id=(partner, tp), device_id_type=MESH)
    for o in range(1, 16):
        pl.semaphore_signal(barrier, inc=1, device_id=(sp, J(0, o % 4, o // 4)), device_id_type=MESH)

    loads = [
        pltpu.make_async_copy(ref.at[0], W.at[176 * i : 176 * i + 176], w_sem.at[i])
        for i, ref in enumerate((wg_ref, wu_ref, wd_ref))
    ]
    for load in loads:
        load.start()

    r0, r1_ = routes_ref[0:1, :], routes_ref[1:2, :]
    ie = iota((32, 128), 0)
    m0 = jnp.where(ie == r0, 1.0, 0.0).astype(F32)
    m1 = jnp.where(ie == r1_, 1.0, 0.0).astype(F32)
    before = jnp.where(iota((128, 128), 0) < iota((128, 128), 1), 1.0, 0.0).astype(BF16)
    earlier = dot((m0 + m1).astype(BF16), before, 1, 0)
    t0 = r0.astype(F32) * 16.0 + jnp.sum(earlier * m0, axis=0, keepdims=True)
    t1 = r1_.astype(F32) * 16.0 + jnp.sum(earlier * m1, axis=0, keepdims=True)
    ir = iota((512, 128), 0).astype(F32)
    p0 = jnp.where(ir == t0, 1.0, 0.0)
    p1 = jnp.where(ir == t1, 1.0, 0.0)
    cot = cot_ref[...].astype(F32)
    c0 = (columns_of(weight_ref[0:1, :]) * cot).astype(BF16)
    c1 = (columns_of(weight_ref[1:2, :]) * cot).astype(BF16)
    rows = dot((p0 + p1).astype(BF16), mi_ref[...], 1, 0).astype(BF16)
    cots = (dot(p0.astype(BF16), c0, 1, 0) + dot(p1.astype(BF16), c1, 1, 0)).astype(BF16)
    S[:, 0] = rows.reshape(32, 16, 128)
    S[:, 1] = cots.reshape(32, 16, 128)

    pl.semaphore_wait(barrier, 46)

    send(S.at[partner], X.at[tp, c], sA, rA.at[0], (partner, tp))
    for r in ORDER[1:]:
        d = (16 - r) % 16
        q = PLACE[r] * 2
        for core in range(2):
            dest = chip(d, core)
            send(S.at[dest], X.at[tp, q + c], sA, rA.at[q // K], (dest, tp))
    X[tp, c] = S[sp]

    opt = jnp.transpose(jnp.pad(op_ref[...].astype(F32), ((0, 64), (0, 64))))
    lane = iota((32, 128), 1)
    OB[sp] = jnp.where(lane < 64, opt[0:32], pltpu.roll(opt[32:64], 64, 1)).astype(BF16)
    send(OB.at[sp], OB.at[sp], sO, rO, (partner, tp))
    for d in range(1, 16):
        for core in range(2):
            send(OB.at[sp], OB.at[sp], sO, rO, (chip(d, core), tp))

    k0, k1 = columns_of(t0), columns_of(t1)
    for n in range(4):
        il = (iota((128, 128), 1) + 128 * n).astype(F32)
        PT[:, 128 * n : 128 * n + 128] = jnp.where((k0 == il) | (k1 == il), 1.0, 0.0).astype(BF16)

    TT[...] = jnp.zeros_like(TT)
    TT[0:31, 0:64] = taps_ref[...].astype(F32)
    TT[31:32, 0:64] = gain_ref[...]
    tt = jnp.transpose(TT[...])
    gain = jnp.broadcast_to(tt[0:64, 31:32], (64, 128))
    for o in range(31):
        TB[o] = jnp.broadcast_to(tt[0:64, o : o + 1], (64, 128))
    normed = (co_ref[...].astype(F32) - mean_ref[...]) * rstd_ref[...]
    scaled = normed * gain
    sig = jax.nn.sigmoid(scaled)
    NM[...] = normed
    FC[...] = sig * (1.0 + scaled * (1.0 - sig)) * gain
    MX[...] = (scaled * sig).astype(BF16)
    SB[...] = jnp.zeros_like(SB)

    def q0(g, h):
        return g * K + h * HK

    def second(g, h, k):
        q = q0(g, h)
        piece = X.at[J(h, FO[k], 0), q : q + HK]
        send(piece, piece, sB, b2.at[g, h, k, 0], (sp, J(h, 0, 1)))
        send(piece, piece, sB, b2.at[g, h, k, 1], (sp, J(h, 0, 3)))

    def pass_on(g, h, k):
        q, fo = q0(g, h), FO[k]
        wait(X.at[J(h, fo, 3), q : q + HK], b2.at[g, h, k, 0])
        half = X.at[J(h, fo, 3), q : q + QK]
        send(half, half, sB, b2f.at[g, h, k, 0], (sp, J(h, 0, 1)))
        wait(X.at[J(h, fo, 1), q : q + HK], b2.at[g, h, k, 1])
        half = X.at[J(h, fo, 1), q + QK : q + HK]
        send(half, half, sB, b2f.at[g, h, k, 1], (sp, J(h, 0, 3)))

    def B0(g):
        first = 1 if g == 0 else 0
        wait(X.at[0, g * K + first : g * K + K], rA.at[g])
        for h in range(2):
            q = q0(g, h)
            piece = X.at[tp, q : q + HK]
            send(piece, piece, sB, b1.at[g, h, 0], (sp, J(h, 1, 0)))
            send(piece, piece, sB, b1.at[g, h, 1], (sp, J(h, 3, 0)))
            second(g, h, 0)

    def B1(g):
        for h in range(2):
            q = q0(g, h)
            own = J(h, 3, 0)
            wait(X.at[own, q : q + HK], b1.at[g, h, 0])
            half = X.at[own, q : q + QK]
            send(half, half, sB, b1f.at[g, h, 0], (sp, J(h, 1, 0)))
            own = J(h, 1, 0)
            wait(X.at[own, q : q + HK], b1.at[g, h, 1])
            half = X.at[own, q + QK : q + HK]
            send(half, half, sB, b1f.at[g, h, 1], (sp, J(h, 3, 0)))
            second(g, h, 1)
            second(g, h, 2)
        for h in range(2):
            pass_on(g, h, 0)

    def B2(g):
        for h in range(2):
            q = q0(g, h)
            own = J(h, 2, 0)
            wait(X.at[own, q : q + QK], b1f.at[g, h, 0])
            wait(X.at[own, q + QK : q + HK], b1f.at[g, h, 1])
            second(g, h, 3)
        for h in range(2):
            pass_on(g, h, 1)
            pass_on(g, h, 2)

    def B3(g):
        for h in range(2):
            pass_on(g, h, 3)

    def C(g):
        for h in range(2):
            q = q0(g, h)
            for k in range(4):
                own = J(h, FO[k], 2)
                wait(X.at[own, q : q + QK], b2f.at[g, h, k, 0])
                wait(X.at[own, q + QK : q + HK], b2f.at[g, h, k, 1])
        if g == 0:
            for load in loads:
                load.wait()
        part = []
        for a in range(2):
            part.append(
                jnp.concatenate(
                    [X[j, g * K : g * K + K, a].reshape(128, 128) for j in range(16)], axis=1
                )
            )
        both = dot(W[0:352], part[0], 1, 1)
        hg = dot(W[352:528], part[1], 1, 1)
        gate, up = both[0:176], both[176:352]
        gs = jax.nn.sigmoid(gate)
        act = gate * gs
        cols = slice(128 * g, 128 * g + 128)
        gd = (hg * up * gs * (1.0 + gate * (1.0 - gs))).astype(BF16)
        ud = (hg * act).astype(BF16)
        DT[0:176, cols] = gd
        DT[176:352, cols] = ud
        DT[352:528, cols] = (act * up).astype(BF16)
        partial = dot(DT[0:352, cols], W[0:352], 0, 0)
        for j in range(16):
            yy, xx = j // 4, j % 4
            block = partial[:, 128 * j : 128 * j + 128].astype(BF16)
            PB[g, 0, xx, yy] = block[0:64]
            PB[g, 1, yy, xx] = block[64:128]
        for h in range(2):
            f = (x, y)[h]
            far = (f + 2) % 4
            send(PB.at[g, h, far, 0:2], T1.at[g, h, 0], s1, r1.at[g, h, 0], (sp, J(h, 1, 0)))
            send(PB.at[g, h, far, 2:4], T1.at[g, h, 1], s1, r1.at[g, h, 1], (sp, J(h, 3, 0)))

    def R1(g):
        for h in range(2):
            f = (x, y)[h]
            nxt, prv = (f + 1) % 4, (f + 3) % 4
            wait(T1.at[g, h, 0], r1.at[g, h, 0])
            PB[g, h, nxt, 0:2] = (PB[g, h, nxt, 0:2].astype(F32) + T1[g, h, 0].astype(F32)).astype(BF16)
            send(PB.at[g, h, nxt], T2.at[g, h, 0], s1, r2.at[g, h, 0], (sp, J(h, 1, 0)))
            wait(T1.at[g, h, 1], r1.at[g, h, 1])
            PB[g, h, prv, 2:4] = (PB[g, h, prv, 2:4].astype(F32) + T1[g, h, 1].astype(F32)).astype(BF16)
            send(PB.at[g, h, prv], T2.at[g, h, 1], s1, r2.at[g, h, 1], (sp, J(h, 3, 0)))

    def R2(g):
        for h in range(2):
            f, s = ((x, y), (y, x))[h]
            wait(T2.at[g, h, 0], r2.at[g, h, 0])
            wait(T2.at[g, h, 1], r2.at[g, h, 1])
            Q[g, h] = (
                PB[g, h, f].astype(F32) + T2[g, h, 0].astype(F32) + T2[g, h, 1].astype(F32)
            ).astype(BF16)
            for d in range(1, 4):
                send(Q.at[g, h, (s + d) % 4], V.at[g, h, d - 1], s3, r3.at[g, h], (sp, J(h, 0, d)))

    def R3(g):
        for h in range(2):
            s = (y, x)[h]
            wait(V.at[g, h], r3.at[g, h])
            total = Q[g, h, s].astype(F32)
            for d in range(3):
                total = total + V[g, h, d].astype(F32)
            FN[g, h] = total.astype(BF16).reshape(HK, 16, 128)
            for k in range(HK):
                q = q0(g, h) + k
                r = ORDER[q // 2]
                if r == 0:
                    continue
                send(FN.at[g, h, k], RT.at[sp], sR, rR, (chip(r, q % 2), tp))
            if g == 0 and h == 0:
                send(FN.at[0, 0, 1 - c], RT.at[sp], sR, rR, (partner, tp))
                RT[sp] = FN[0, 0, c]

    def grads(lo, hi):
        def step(jp, carry):
            at = pl.ds(pl.multiple_of(jp * 256, 256), 256)
            rhs = jnp.concatenate(
                [X[2 * jp + i, :, 0].reshape(512, 128) for i in range(2)], axis=1
            )
            GO[0:352, at] = dot(DT[0:352], rhs, 1, 0).astype(BF16)
            rhs = jnp.concatenate(
                [X[2 * jp + i, :, 1].reshape(512, 128) for i in range(2)], axis=1
            )
            GO[352:528, at] = dot(DT[352:528], rhs, 1, 0).astype(BF16)
            return carry

        lax.fori_loop(lo, hi, step, 0)

    for t in range(G + 7):
        for fn, lag in ((B0, 0), (B1, 1), (B2, 2), (B3, 3), (R3, 7), (R2, 6), (R1, 5), (C, 4)):
            if 0 <= t - lag < G:
                fn(t - lag)
        if t >= G + 3:
            n = t - G - 3
            grads(2 * n, 2 * n + 2)

    stores = [
        pltpu.make_async_copy(GO.at[176 * i : 176 * i + 176], ref.at[0], o_sem.at[i])
        for i, ref in enumerate((gate_out, up_out, down_out))
    ]
    for store in stores:
        store.start()

    wait(OB.at[0:31], rO)
    for j in range(16):
        a, b = OB[2 * j].astype(F32), OB[2 * j + 1].astype(F32)
        OPT[0:32, 128 * j : 128 * j + 128] = jnp.where(lane < 64, a, pltpu.roll(b, 64, 1)).astype(BF16)
        OPT[32:64, 128 * j : 128 * j + 128] = jnp.where(lane < 64, pltpu.roll(a, 64, 1), b).astype(BF16)

    wait(RT.at[0:31], rR)
    mine = dot(PT[...], RT[...].reshape(512, 128), 1, 0)
    stream = (cot_ref[...].astype(F32) + mine).astype(BF16)
    FS[tp] = stream
    stream_out[...] = stream
    for o in range(1, 16):
        send(FS.at[tp], FS.at[tp], sF, rF, (sp, J(0, o % 4, o // 4)))
    wait(FS.at[0:15], rF)
    full = jnp.concatenate([FS[j] for j in range(16)], axis=1)

    gt = dot(MX[...], full, 1, 0)
    for k in range(16):
        top, bottom = gt[0:32, 128 * k : 128 * k + 128], gt[32:64, 128 * k : 128 * k + 128]
        GP[0, k] = jnp.where(lane < 64, top, pltpu.roll(bottom, 64, 1)).astype(BF16)
        GP[1, k] = jnp.where(lane < 64, pltpu.roll(top, 64, 1), bottom).astype(BF16)
    send(GP.at[1 - c], GI, sD, rD, (partner, tp))

    ng = dot(OPT[...], full, 1, 1) * FC[...]
    normed = NM[...]
    SB[0:1, :] = jnp.sum(ng, axis=0, keepdims=True)
    SB[1:2, :] = jnp.sum(ng * normed, axis=0, keepdims=True)
    for o in range(1, 16):
        send(SB, SR.at[tp], sS, rS, (sp, J(0, o % 4, o // 4)))
    SR[tp] = SB[...]

    wait(GI, rD)
    GS[...] = (GP[c].astype(F32) + GI[...].astype(F32)).astype(BF16)
    for d in range(1, 16):
        send(GS.at[(z + d) % 16], GR.at[z], sG, rG, (chip(d, c), tp))
    GR[z] = GS[z]

    wait(SR.at[0:15], rS)
    sums = jnp.sum(SR[...], axis=0) * (1.0 / 1024.0)
    cg = rstd_ref[...] * (ng - sums[0:1, :] - normed * sums[1:2, :])
    CG[...] = cg
    send(CG, HB, sH, rH, ((sp + 31) % 32, tp))
    wait(HB, rH)
    halo = jnp.where(sp == 31, 0.0, HB[...])
    lanes = iota((64, 128), 1)
    unit = TB[30] * cg
    for o in range(30):
        lead = 30 - o
        unit = unit + TB[o] * pltpu.roll(jnp.where(lanes >= lead, cg, halo), 128 - lead, 1)
    vs = jax.nn.sigmoid(vg_ref[...].astype(F32))
    value_out[...] = (unit * vs).astype(BF16)
    gating_out[...] = (unit * vv_ref[...].astype(F32) * vs * (1.0 - vs)).astype(BF16)

    wait(GR.at[0:15], rG)
    total = GR[0].astype(F32)
    for k in range(1, 16):
        total = total + GR[k].astype(F32)
    TT[0:32, :] = total
    TT[32:64, :] = pltpu.roll(total, 64, 1)
    proj_out[...] = jnp.transpose(TT[...])[0:64, 0:64]

    wait(S.at[0:31], sA)
    wait(OB.at[0:31], sO)
    wait(X.at[0:15], sB)
    wait(PB.at[0:3], s1)
    wait(Q.at[0:3], s3)
    wait(RT.at[0:31], sR)
    wait(FS.at[0:15], sF)
    wait(GI, sD)
    wait(GR.at[0:15], sG)
    wait(SR.at[0:15], sS)
    wait(HB, sH)
    for store in stores:
        store.wait()


def shards(
    moe_input, cotangent, routes, route_weight, w_gate, w_up, w_down, v_value, v_gate, conv_out,
    row_mean, row_rstd, ln_gain, taps, out_proj,
):
    vmem = pl.BlockSpec(memory_space=pltpu.VMEM)
    hbm = pl.BlockSpec(memory_space=pltpu.HBM)
    dma = pltpu.SemaphoreType.DMA
    v = pltpu.VMEM
    out = pl.pallas_call(
        kernel,
        out_shape=(
            jax.ShapeDtypeStruct((1, 176, 2048), BF16),
            jax.ShapeDtypeStruct((1, 176, 2048), BF16),
            jax.ShapeDtypeStruct((1, 176, 2048), BF16),
            jax.ShapeDtypeStruct((64, 64), F32),
            jax.ShapeDtypeStruct((128, 128), BF16),
            jax.ShapeDtypeStruct((64, 128), BF16),
            jax.ShapeDtypeStruct((64, 128), BF16),
        ),
        in_specs=[vmem] * 4 + [hbm] * 3 + [vmem] * 8,
        out_specs=(hbm, hbm, hbm, vmem, vmem, vmem, vmem),
        scratch_shapes=[
            v((32, 2, 16, 128), BF16),
            v((16, 32, 2, 16, 128), BF16),
            v((528, 2048), BF16),
            v((528, 2048), BF16),
            v((G, 2, 4, 4, 64, 128), BF16),
            v((G, 2, 2, 2, 64, 128), BF16),
            v((G, 2, 2, 4, 64, 128), BF16),
            v((G, 2, 4, 64, 128), BF16),
            v((G, 2, 3, 64, 128), BF16),
            v((G, 2, HK, 16, 128), BF16),
            v((32, 16, 128), BF16),
            v((16, 128, 128), BF16),
            v((528, 512), BF16),
            v((128, 512), BF16),
            v((32, 32, 128), BF16),
            v((64, 2048), BF16),
            v((128, 128), F32),
            v((31, 64, 128), F32),
            v((64, 128), F32),
            v((64, 128), F32),
            v((64, 128), BF16),
            v((2, 16, 32, 128), BF16),
            v((16, 32, 128), BF16),
            v((16, 32, 128), BF16),
            v((16, 32, 128), BF16),
            v((8, 128), F32),
            v((16, 8, 128), F32),
            v((64, 128), F32),
            v((64, 128), F32),
            dma((3,)), dma((3,)),
            dma(()), dma((G,)),
            dma(()), dma((G, 2, 2)), dma((G, 2, 2)), dma((G, 2, 4, 2)), dma((G, 2, 4, 2)),
            dma(()), dma((G, 2, 2)), dma((G, 2, 2)), dma(()), dma((G, 2)),
            dma(()), dma(()), dma(()), dma(()),
            dma(()), dma(()), dma(()), dma(()), dma(()), dma(()),
            dma(()), dma(()), dma(()), dma(()),
        ],
        compiler_params=pltpu.CompilerParams(
            collective_id=0, has_side_effects=True, vmem_limit_bytes=56 * 1024 * 1024
        ),
    )(
        routes.T, route_weight.T, moe_input, cotangent, w_gate, w_up, w_down, v_value.T, v_gate.T,
        conv_out.T, row_mean.reshape(1, 128), row_rstd.reshape(1, 128), ln_gain.reshape(1, 64), taps,
        out_proj,
    )
    gate_g, up_g, down_g, proj_g, stream, value_t, gating_t = out
    return gate_g, up_g, down_g, proj_g, stream, value_t.T, gating_t.T


def solution(mesh):
    return jax.shard_map(
        shards,
        mesh=mesh,
        in_specs=(
            P("sp", "tp"),
            P("sp", "tp"),
            P("sp", None),
            P("sp", None),
            P("sp", "tp", None),
            P("sp", "tp", None),
            P("sp", "tp", None),
            P("sp", "tp"),
            P("sp", "tp"),
            P("sp", "tp"),
            P("sp"),
            P("sp"),
            P("tp"),
            P(None, "tp"),
            P("sp", "tp"),
        ),
        out_specs=(
            P("sp", "tp", None),
            P("sp", "tp", None),
            P("sp", "tp", None),
            P("sp", "tp"),
            P("sp", "tp"),
            P("sp", "tp"),
            P("sp", "tp"),
        ),
        check_vma=False,
    )
```

```python
import jax
import jax.numpy as jnp
from jax import lax
from jax.experimental import pallas as pl
from jax.experimental.pallas import tpu as pltpu
from jax.sharding import PartitionSpec as P

PEERS = (1, 3, 4, 12, 5, 7, 13, 15, 2, 8, 6, 9, 11, 14, 10)
MESH = pl.DeviceIdType.MESH
F32 = jnp.float32
BF16 = jnp.bfloat16
ORDER = (0, 1, 15, 2, 8, 7, 9, 6, 10, 5, 11, 4, 12, 3, 13, 14)
PLACE = {r: i for i, r in enumerate(ORDER)}
G = 4
STRIDE = 1
STEPS = (("B0", 0), ("B1", 2), ("B2", 4), ("B3", 6), ("R3", 14), ("R2", 12), ("R1", 10), ("C", 8))
OUT_AT = 3
K = 32 // G
HK = K // 2
QK = K // 4
RG = 16 * K
RH = 16 * HK
FO = (0, 3, 1, 2)


def dot(a, b, ca, cb):
    return lax.dot_general(a, b, (((ca,), (cb,)), ((), ())), preferred_element_type=F32)


def iota(shape, dim):
    return lax.broadcasted_iota(jnp.int32, shape, dim)


def columns_of(row):
    return jnp.transpose(jnp.broadcast_to(row, (128, 128)))


def kernel(
    routes_ref, weight_ref, mi_ref, cot_ref, wg_ref, wu_ref, wd_ref, vv_ref, vg_ref, co_ref,
    mean_ref, rstd_ref, gain_ref, taps_ref, op_ref,
    GO, proj_out, stream_out, value_out, gating_out,
    S, X, W, PB, T1, T2, Q, V, FN, RT, FS, DT, PT, OB, OPT, TT, TB, NM, FC, MX,
    GP, GI, GS, GR, SB, SR, CG, HB,
    w_sem, sA, rA, sB, b1, b1f, b2, b2f, s1, r1, r2, s3, r3, sR, rR, sF, rF,
    sO, rO, sD, rD, sG, rG, sS, rS, sH, rH,
):
    sp, tp = lax.axis_index("sp"), lax.axis_index("tp")
    z, c = sp // 2, sp % 2
    y, x = tp // 4, tp % 4
    partner = z * 2 + 1 - c

    def J(h, fo, so):
        yy, xx = (so, fo) if h == 0 else (fo, so)
        return ((y + yy) % 4) * 4 + (x + xx) % 4

    def chip(d, core):
        return ((z + d) % 16) * 2 + core

    def send(src, dst, ssem, rsem, dev):
        pltpu.make_async_remote_copy(
            src_ref=src, dst_ref=dst, send_sem=ssem, recv_sem=rsem, device_id=dev, device_id_type=MESH
        ).start()

    def wait(ref, sem):
        pltpu.make_async_copy(ref, ref, sem).wait()

    barrier = pltpu.get_barrier_semaphore()
    for d in range(16):
        for core in range(2):
            if d == 0:
                continue
            pl.semaphore_signal(barrier, inc=1, device_id=(chip(d, core), tp), device_id_type=MESH)
    pl.semaphore_signal(barrier, inc=1, device_id=(partner, tp), device_id_type=MESH)
    for o in range(1, 16):
        pl.semaphore_signal(barrier, inc=1, device_id=(sp, J(0, o % 4, o // 4)), device_id_type=MESH)

    loads = [
        pltpu.make_async_copy(ref.at[0], W.at[176 * i : 176 * i + 176], w_sem.at[i])
        for i, ref in enumerate((wg_ref, wu_ref, wd_ref))
    ]
    for load in loads:
        load.start()

    r0, r1_ = routes_ref[0:1, :], routes_ref[1:2, :]
    ie = iota((32, 128), 0)
    m0 = jnp.where(ie == r0, 1.0, 0.0).astype(F32)
    m1 = jnp.where(ie == r1_, 1.0, 0.0).astype(F32)
    before = jnp.where(iota((128, 128), 0) < iota((128, 128), 1), 1.0, 0.0).astype(BF16)
    earlier = dot((m0 + m1).astype(BF16), before, 1, 0)
    t0 = r0.astype(F32) * 16.0 + jnp.sum(earlier * m0, axis=0, keepdims=True)
    t1 = r1_.astype(F32) * 16.0 + jnp.sum(earlier * m1, axis=0, keepdims=True)
    ir = iota((512, 128), 0).astype(F32)
    p0 = jnp.where(ir == t0, 1.0, 0.0)
    p1 = jnp.where(ir == t1, 1.0, 0.0)
    cot = cot_ref[...].astype(F32)
    c0 = (columns_of(weight_ref[0:1, :]) * cot).astype(BF16)
    c1 = (columns_of(weight_ref[1:2, :]) * cot).astype(BF16)
    rows = dot((p0 + p1).astype(BF16), mi_ref[...], 1, 0).astype(BF16)
    cots = (dot(p0.astype(BF16), c0, 1, 0) + dot(p1.astype(BF16), c1, 1, 0)).astype(BF16)
    S[:, 0] = rows.reshape(32, 16, 128)
    S[:, 1] = cots.reshape(32, 16, 128)

    pl.semaphore_wait(barrier, 46)

    send(S.at[partner], X.at[tp, c], sA, rA.at[0], (partner, tp))
    for r in ORDER[1:]:
        d = (16 - r) % 16
        q = PLACE[r] * 2
        for core in range(2):
            dest = chip(d, core)
            send(S.at[dest], X.at[tp, q + c], sA, rA.at[q // K], (dest, tp))
    X[tp, c] = S[sp]

    opt = jnp.transpose(jnp.pad(op_ref[...].astype(F32), ((0, 64), (0, 64))))
    lane = iota((32, 128), 1)
    OB[sp] = jnp.where(lane < 64, opt[0:32], pltpu.roll(opt[32:64], 64, 1)).astype(BF16)

    def share_projection():
        send(OB.at[sp], OB.at[sp], sO, rO, (partner, tp))
        for d in range(1, 16):
            for core in range(2):
                send(OB.at[sp], OB.at[sp], sO, rO, (chip(d, core), tp))

    k0, k1 = columns_of(t0), columns_of(t1)
    for n in range(4):
        il = (iota((128, 128), 1) + 128 * n).astype(F32)
        PT[:, 128 * n : 128 * n + 128] = jnp.where((k0 == il) | (k1 == il), 1.0, 0.0).astype(BF16)

    TT[...] = jnp.zeros_like(TT)
    TT[0:31, 0:64] = taps_ref[...].astype(F32)
    TT[31:32, 0:64] = gain_ref[...]
    tt = jnp.transpose(TT[...])
    gain = jnp.broadcast_to(tt[0:64, 31:32], (64, 128))
    for o in range(31):
        TB[o] = jnp.broadcast_to(tt[0:64, o : o + 1], (64, 128))
    normed = (co_ref[...].astype(F32) - mean_ref[...]) * rstd_ref[...]
    scaled = normed * gain
    sig = jax.nn.sigmoid(scaled)
    NM[...] = normed
    FC[...] = sig * (1.0 + scaled * (1.0 - sig)) * gain
    MX[...] = (scaled * sig).astype(BF16)
    SB[...] = jnp.zeros_like(SB)

    def q0(g, h):
        return g * K + h * HK

    def second(g, h, k):
        q = q0(g, h)
        piece = X.at[J(h, FO[k], 0), q : q + HK]
        send(piece, piece, sB, b2.at[g, h, k, 0], (sp, J(h, 0, 1)))
        send(piece, piece, sB, b2.at[g, h, k, 1], (sp, J(h, 0, 3)))

    def pass_on(g, h, k):
        q, fo = q0(g, h), FO[k]
        wait(X.at[J(h, fo, 3), q : q + HK], b2.at[g, h, k, 0])
        half = X.at[J(h, fo, 3), q : q + QK]
        send(half, half, sB, b2f.at[g, h, k, 0], (sp, J(h, 0, 1)))
        wait(X.at[J(h, fo, 1), q : q + HK], b2.at[g, h, k, 1])
        half = X.at[J(h, fo, 1), q + QK : q + HK]
        send(half, half, sB, b2f.at[g, h, k, 1], (sp, J(h, 0, 3)))

    def B0(g):
        first = 1 if g == 0 else 0
        wait(X.at[0, g * K + first : g * K + K], rA.at[g])
        for h in range(2):
            q = q0(g, h)
            piece = X.at[tp, q : q + HK]
            send(piece, piece, sB, b1.at[g, h, 0], (sp, J(h, 1, 0)))
            send(piece, piece, sB, b1.at[g, h, 1], (sp, J(h, 3, 0)))
            second(g, h, 0)

    def B1(g):
        for h in range(2):
            q = q0(g, h)
            own = J(h, 3, 0)
            wait(X.at[own, q : q + HK], b1.at[g, h, 0])
            half = X.at[own, q : q + QK]
            send(half, half, sB, b1f.at[g, h, 0], (sp, J(h, 1, 0)))
            own = J(h, 1, 0)
            wait(X.at[own, q : q + HK], b1.at[g, h, 1])
            half = X.at[own, q + QK : q + HK]
            send(half, half, sB, b1f.at[g, h, 1], (sp, J(h, 3, 0)))
            second(g, h, 1)
            second(g, h, 2)
        for h in range(2):
            pass_on(g, h, 0)

    def B2(g):
        for h in range(2):
            q = q0(g, h)
            own = J(h, 2, 0)
            wait(X.at[own, q : q + QK], b1f.at[g, h, 0])
            wait(X.at[own, q + QK : q + HK], b1f.at[g, h, 1])
            second(g, h, 3)
        for h in range(2):
            pass_on(g, h, 1)
            pass_on(g, h, 2)

    def B3(g):
        for h in range(2):
            pass_on(g, h, 3)

    def C(g):
        for h in range(2):
            q = q0(g, h)
            for k in range(4):
                own = J(h, FO[k], 2)
                wait(X.at[own, q : q + QK], b2f.at[g, h, k, 0])
                wait(X.at[own, q + QK : q + HK], b2f.at[g, h, k, 1])
        if g == 0:
            for load in loads:
                load.wait()
        part = []
        for a in range(2):
            part.append(
                jnp.concatenate(
                    [X[j, g * K : g * K + K, a].reshape(RG, 128) for j in range(16)], axis=1
                )
            )
        both = dot(W[0:352], part[0], 1, 1)
        hg = dot(W[352:528], part[1], 1, 1)
        gate, up = both[0:176], both[176:352]
        gs = jax.nn.sigmoid(gate)
        act = gate * gs
        cols = slice(RG * g, RG * g + RG)
        gd = (hg * up * gs * (1.0 + gate * (1.0 - gs))).astype(BF16)
        ud = (hg * act).astype(BF16)
        DT[0:176, cols] = gd
        DT[176:352, cols] = ud
        DT[352:528, cols] = (act * up).astype(BF16)
        partial = dot(DT[0:352, cols], W[0:352], 0, 0)
        for j in range(16):
            yy, xx = j // 4, j % 4
            block = partial[:, 128 * j : 128 * j + 128].astype(BF16)
            PB[g, 0, xx, yy] = block[0:RH]
            PB[g, 1, yy, xx] = block[RH:RG]
        for h in range(2):
            f = (x, y)[h]
            far = (f + 2) % 4
            send(PB.at[g, h, far, 0:2], T1.at[g, h, 0], s1, r1.at[g, h, 0], (sp, J(h, 1, 0)))
            send(PB.at[g, h, far, 2:4], T1.at[g, h, 1], s1, r1.at[g, h, 1], (sp, J(h, 3, 0)))

    def R1(g):
        for h in range(2):
            f = (x, y)[h]
            nxt, prv = (f + 1) % 4, (f + 3) % 4
            wait(T1.at[g, h, 0], r1.at[g, h, 0])
            PB[g, h, nxt, 0:2] = (PB[g, h, nxt, 0:2].astype(F32) + T1[g, h, 0].astype(F32)).astype(BF16)
            send(PB.at[g, h, nxt], T2.at[g, h, 0], s1, r2.at[g, h, 0], (sp, J(h, 1, 0)))
            wait(T1.at[g, h, 1], r1.at[g, h, 1])
            PB[g, h, prv, 2:4] = (PB[g, h, prv, 2:4].astype(F32) + T1[g, h, 1].astype(F32)).astype(BF16)
            send(PB.at[g, h, prv], T2.at[g, h, 1], s1, r2.at[g, h, 1], (sp, J(h, 3, 0)))

    def R2(g):
        for h in range(2):
            f, s = ((x, y), (y, x))[h]
            wait(T2.at[g, h, 0], r2.at[g, h, 0])
            wait(T2.at[g, h, 1], r2.at[g, h, 1])
            Q[g, h] = (
                PB[g, h, f].astype(F32) + T2[g, h, 0].astype(F32) + T2[g, h, 1].astype(F32)
            ).astype(BF16)
            for d in range(1, 4):
                send(Q.at[g, h, (s + d) % 4], V.at[g, h, d - 1], s3, r3.at[g, h], (sp, J(h, 0, d)))

    def R3(g):
        for h in range(2):
            s = (y, x)[h]
            wait(V.at[g, h], r3.at[g, h])
            total = Q[g, h, s].astype(F32)
            for d in range(3):
                total = total + V[g, h, d].astype(F32)
            FN[g, h] = total.astype(BF16).reshape(HK, 16, 128)
            for k in range(HK):
                q = q0(g, h) + k
                r = ORDER[q // 2]
                if r == 0:
                    continue
                send(FN.at[g, h, k], RT.at[sp], sR, rR, (chip(r, q % 2), tp))
            if g == 0 and h == 0:
                send(FN.at[0, 0, 1 - c], RT.at[sp], sR, rR, (partner, tp))
                RT[sp] = FN[0, 0, c]

    def grads(lo, hi):
        def step(jp, carry):
            at = pl.ds(pl.multiple_of(jp * 256, 256), 256)
            rhs = jnp.concatenate(
                [X[2 * jp + i, :, 0].reshape(512, 128) for i in range(2)], axis=1
            )
            GO[0:352, at] = dot(DT[0:352], rhs, 1, 0).astype(BF16)
            rhs = jnp.concatenate(
                [X[2 * jp + i, :, 1].reshape(512, 128) for i in range(2)], axis=1
            )
            GO[352:528, at] = dot(DT[352:528], rhs, 1, 0).astype(BF16)
            return carry

        lax.fori_loop(lo, hi, step, 0)

    plan = {"B0": B0, "B1": B1, "B2": B2, "B3": B3, "C": C, "R1": R1, "R2": R2, "R3": R3}
    left = 0
    for t in range(STRIDE * (G - 1) + 1 + max(lag for _, lag in STEPS)):
        for name, lag in STEPS:
            g, off = (t - lag) // STRIDE, (t - lag) % STRIDE
            if off == 0 and 0 <= g < G:
                plan[name](g)
        if t == OUT_AT:
            share_projection()
        if t >= STRIDE * (G - 1) + STEPS[-1][1] and left < 8:
            grads(left, left + 2)
            left += 2

    wait(OB.at[0:31], rO)
    for j in range(16):
        a, b = OB[2 * j].astype(F32), OB[2 * j + 1].astype(F32)
        OPT[j, 0:32] = jnp.where(lane < 64, a, pltpu.roll(b, 64, 1)).astype(BF16)
        OPT[j, 32:64] = jnp.where(lane < 64, pltpu.roll(a, 64, 1), b).astype(BF16)

    wait(RT.at[0:31], rR)
    mine = dot(PT[...], RT[...].reshape(512, 128), 1, 0)
    stream = (cot_ref[...].astype(F32) + mine).astype(BF16)
    FS[tp] = stream
    stream_out[...] = stream
    for o in PEERS:
        send(FS.at[tp], FS.at[tp], sF, rF.at[o], (sp, J(0, o % 4, o // 4)))
    acc = jnp.zeros((64, 128), F32)

    def pair_sum(o):
        k = J(0, -o % 4, -(o // 4) % 4)
        wait(GI.at[k], rD.at[o])
        GS[k] = (GP[c, k].astype(F32) + GI[k].astype(F32)).astype(BF16)

        @pl.when(k == z)
        def _():
            GR[z] = GS[z]

        @pl.when(k != z)
        def _():
            send(GS.at[k], GR.at[z], sG, rG, (2 * k + c, tp))

    pieces = (0,) + PEERS
    for n, o in enumerate(pieces):
        k = J(0, -o % 4, -(o // 4) % 4)
        if o:
            wait(FS.at[k], rF.at[o])
        piece = FS[k]
        gt = dot(MX[...], piece, 1, 0)
        top, bottom = gt[0:32], gt[32:64]
        GP[0, k] = jnp.where(lane < 64, top, pltpu.roll(bottom, 64, 1)).astype(BF16)
        GP[1, k] = jnp.where(lane < 64, pltpu.roll(top, 64, 1), bottom).astype(BF16)
        send(GP.at[1 - c, k], GI.at[k], sD, rD.at[o], (partner, tp))
        acc = acc + dot(OPT[k], piece, 1, 1)
        if n >= 4:
            pair_sum(pieces[n - 4])

    ng = acc * FC[...]
    normed = NM[...]
    SB[0:1, :] = jnp.sum(ng, axis=0, keepdims=True)
    SB[1:2, :] = jnp.sum(ng * normed, axis=0, keepdims=True)
    for o in range(1, 16):
        send(SB, SR.at[tp], sS, rS, (sp, J(0, o % 4, o // 4)))
    SR[tp] = SB[...]

    for o in pieces[12:]:
        pair_sum(o)

    wait(SR.at[0:15], rS)
    sums = jnp.sum(SR[...], axis=0) * (1.0 / 1024.0)
    cg = rstd_ref[...] * (ng - sums[0:1, :] - normed * sums[1:2, :])
    CG[...] = cg
    send(CG, HB, sH, rH, ((sp + 31) % 32, tp))
    wait(HB, rH)
    halo = jnp.where(sp == 31, 0.0, HB[...])
    lanes = iota((64, 128), 1)
    unit = TB[30] * cg
    for o in range(30):
        lead = 30 - o
        unit = unit + TB[o] * pltpu.roll(jnp.where(lanes >= lead, cg, halo), 128 - lead, 1)
    vs = jax.nn.sigmoid(vg_ref[...].astype(F32))
    value_out[...] = (unit * vs).astype(BF16)
    gating_out[...] = (unit * vv_ref[...].astype(F32) * vs * (1.0 - vs)).astype(BF16)

    wait(GR.at[0:15], rG)
    total = GR[0].astype(F32)
    for k in range(1, 16):
        total = total + GR[k].astype(F32)
    TT[0:32, :] = total
    TT[32:64, :] = pltpu.roll(total, 64, 1)
    proj_out[...] = jnp.transpose(TT[...])[0:64, 0:64]

    wait(S.at[0:31], sA)
    wait(OB.at[0:31], sO)
    wait(X.at[0:15], sB)
    wait(PB.at[:, :, 0:3], s1)
    wait(Q.at[:, :, 0:3], s3)
    wait(RT.at[0:31], sR)
    wait(FS.at[0:15], sF)
    wait(GI, sD)
    wait(GR.at[0:15], sG)
    wait(SR.at[0:15], sS)
    wait(HB, sH)


def finish(
    go, proj, stream, value, gating,
    gate_out, up_out, down_out, proj_out, stream_out, value_out, gating_out, sems,
):
    pairs = [(go.at[176 * i : 176 * i + 176], r.at[0]) for i, r in enumerate((gate_out, up_out, down_out))]
    pairs += [(proj, proj_out), (stream, stream_out), (value, value_out), (gating, gating_out)]
    copies = [pltpu.make_async_copy(a, b, sems.at[i]) for i, (a, b) in enumerate(pairs)]
    for copy in copies:
        copy.start()
    for copy in copies:
        copy.wait()


def shards(
    moe_input, cotangent, routes, route_weight, w_gate, w_up, w_down, v_value, v_gate, conv_out,
    row_mean, row_rstd, ln_gain, taps, out_proj,
):
    vmem = pl.BlockSpec(memory_space=pltpu.VMEM)
    hbm = pl.BlockSpec(memory_space=pltpu.HBM)
    dma = pltpu.SemaphoreType.DMA
    v = pltpu.VMEM
    out = pl.pallas_call(
        kernel,
        out_shape=(
            v((528, 2048), BF16),
            v((64, 64), F32),
            v((128, 128), BF16),
            v((64, 128), BF16),
            v((64, 128), BF16),
        ),
        in_specs=[vmem] * 4 + [hbm] * 3 + [vmem] * 8,
        out_specs=(vmem,) * 5,
        scratch_shapes=[
            v((32, 2, 16, 128), BF16),
            v((16, 32, 2, 16, 128), BF16),
            v((528, 2048), BF16),
            v((G, 2, 4, 4, RH, 128), BF16),
            v((G, 2, 2, 2, RH, 128), BF16),
            v((G, 2, 2, 4, RH, 128), BF16),
            v((G, 2, 4, RH, 128), BF16),
            v((G, 2, 3, RH, 128), BF16),
            v((G, 2, HK, 16, 128), BF16),
            v((32, 16, 128), BF16),
            v((16, 128, 128), BF16),
            v((528, 512), BF16),
            v((128, 512), BF16),
            v((32, 32, 128), BF16),
            v((16, 64, 128), BF16),
            v((128, 128), F32),
            v((31, 64, 128), F32),
            v((64, 128), F32),
            v((64, 128), F32),
            v((64, 128), BF16),
            v((2, 16, 32, 128), BF16),
            v((16, 32, 128), BF16),
            v((16, 32, 128), BF16),
            v((16, 32, 128), BF16),
            v((8, 128), F32),
            v((16, 8, 128), F32),
            v((64, 128), F32),
            v((64, 128), F32),
            dma((3,)),
            dma(()), dma((G,)),
            dma(()), dma((G, 2, 2)), dma((G, 2, 2)), dma((G, 2, 4, 2)), dma((G, 2, 4, 2)),
            dma(()), dma((G, 2, 2)), dma((G, 2, 2)), dma(()), dma((G, 2)),
            dma(()), dma(()), dma(()), dma((16,)),
            dma(()), dma(()), dma(()), dma((16,)), dma(()), dma(()),
            dma(()), dma(()), dma(()), dma(()),
        ],
        compiler_params=pltpu.CompilerParams(
            collective_id=0, has_side_effects=True, vmem_limit_bytes=56 * 1024 * 1024
        ),
    )(
        routes.T, route_weight.T, moe_input, cotangent, w_gate, w_up, w_down, v_value.T, v_gate.T,
        conv_out.T, row_mean.reshape(1, 128), row_rstd.reshape(1, 128), ln_gain.reshape(1, 64), taps,
        out_proj,
    )
    shapes = ((1, 176, 2048),) * 3 + ((64, 64), (128, 128), (64, 128), (64, 128))
    kinds = (BF16, BF16, BF16, F32, BF16, BF16, BF16)
    out = pl.pallas_call(
        finish,
        out_shape=tuple(jax.ShapeDtypeStruct(a, b) for a, b in zip(shapes, kinds)),
        in_specs=[vmem] * 5,
        out_specs=(hbm,) * 7,
        scratch_shapes=[dma((7,))],
        compiler_params=pltpu.CompilerParams(vmem_limit_bytes=4 * 1024 * 1024),
    )(*out)
    gate_g, up_g, down_g, proj_g, stream, value_t, gating_t = out
    return gate_g, up_g, down_g, proj_g, stream, value_t.T, gating_t.T


def solution(mesh):
    return jax.shard_map(
        shards,
        mesh=mesh,
        in_specs=(
            P("sp", "tp"),
            P("sp", "tp"),
            P("sp", None),
            P("sp", None),
            P("sp", "tp", None),
            P("sp", "tp", None),
            P("sp", "tp", None),
            P("sp", "tp"),
            P("sp", "tp"),
            P("sp", "tp"),
            P("sp"),
            P("sp"),
            P("tp"),
            P(None, "tp"),
            P("sp", "tp"),
        ),
        out_specs=(
            P("sp", "tp", None),
            P("sp", "tp", None),
            P("sp", "tp", None),
            P("sp", "tp"),
            P("sp", "tp"),
            P("sp", "tp"),
            P("sp", "tp"),
        ),
        check_vma=False,
    )
```

```python
import jax
import jax.numpy as jnp
from jax import lax
from jax.experimental import pallas as pl
from jax.experimental.pallas import tpu as pltpu
from jax.sharding import PartitionSpec as P

PEERS = (1, 3, 4, 12, 5, 7, 13, 15, 2, 8, 6, 9, 11, 14, 10)
MESH = pl.DeviceIdType.MESH
F32 = jnp.float32
BF16 = jnp.bfloat16
ORDER = (0, 1, 15, 2, 8, 7, 9, 6, 10, 5, 11, 4, 12, 3, 13, 14)
PLACE = {r: i for i, r in enumerate(ORDER)}
G = 4
STRIDE = 1
STEPS = (("R3", 14), ("R2", 12), ("R1", 10), ("B3", 6), ("B2", 4), ("B1", 2), ("B0", 0), ("C", 8))
OUT_AT = 3
K = 32 // G
HK = K // 2
QK = K // 4
RG = 16 * K
RH = 16 * HK


def dot(a, b, ca, cb):
    return lax.dot_general(a, b, (((ca,), (cb,)), ((), ())), preferred_element_type=F32)


def iota(shape, dim):
    return lax.broadcasted_iota(jnp.int32, shape, dim)


def columns_of(row):
    return jnp.transpose(jnp.broadcast_to(row, (128, 128)))


def kernel(
    routes_ref, weight_ref, mi_ref, cot_ref, wg_ref, wu_ref, wd_ref, vv_ref, vg_ref, co_ref,
    mean_ref, rstd_ref, gain_ref, taps_ref, op_ref,
    GO, proj_out, stream_out, value_out, gating_out,
    S, X, W, PB, T1, T2, Q, V, FN, RT, FS, DT, PT, OB, OPT, TT, TB, NM, FC, MX,
    GP, GI, GS, GR, SB, SR, CG, HB,
    w_sem, sA, rA, sB, b1, b1f, b2, b2f, s1, r1, r2, s3, r3, sR, rR, sF, rF,
    sO, rO, sD, rD, sG, rG, sS, rS, sH, rH,
):
    sp, tp = lax.axis_index("sp"), lax.axis_index("tp")
    z, c = sp // 2, sp % 2
    y, x = tp // 4, tp % 4
    partner = z * 2 + 1 - c

    def J(h, fo, so):
        yy, xx = (so, fo) if h == 0 else (fo, so)
        return ((y + yy) % 4) * 4 + (x + xx) % 4

    def chip(d, core):
        return ((z + d) % 16) * 2 + core

    def send(src, dst, ssem, rsem, dev):
        pltpu.make_async_remote_copy(
            src_ref=src, dst_ref=dst, send_sem=ssem, recv_sem=rsem, device_id=dev, device_id_type=MESH
        ).start()

    def wait(ref, sem):
        pltpu.make_async_copy(ref, ref, sem).wait()

    barrier = pltpu.get_barrier_semaphore()
    for d in range(16):
        for core in range(2):
            if d == 0:
                continue
            pl.semaphore_signal(barrier, inc=1, device_id=(chip(d, core), tp), device_id_type=MESH)
    pl.semaphore_signal(barrier, inc=1, device_id=(partner, tp), device_id_type=MESH)
    for o in range(1, 16):
        pl.semaphore_signal(barrier, inc=1, device_id=(sp, J(0, o % 4, o // 4)), device_id_type=MESH)

    loads = [
        pltpu.make_async_copy(ref.at[0], W.at[176 * i : 176 * i + 176], w_sem.at[i])
        for i, ref in enumerate((wg_ref, wu_ref, wd_ref))
    ]
    for load in loads:
        load.start()

    r0, r1_ = routes_ref[0:1, :], routes_ref[1:2, :]
    ie = iota((32, 128), 0)
    m0 = jnp.where(ie == r0, 1.0, 0.0).astype(F32)
    m1 = jnp.where(ie == r1_, 1.0, 0.0).astype(F32)
    before = jnp.where(iota((128, 128), 0) < iota((128, 128), 1), 1.0, 0.0).astype(BF16)
    earlier = dot((m0 + m1).astype(BF16), before, 1, 0)
    t0 = r0.astype(F32) * 16.0 + jnp.sum(earlier * m0, axis=0, keepdims=True)
    t1 = r1_.astype(F32) * 16.0 + jnp.sum(earlier * m1, axis=0, keepdims=True)
    ir = iota((512, 128), 0).astype(F32)
    p0 = jnp.where(ir == t0, 1.0, 0.0)
    p1 = jnp.where(ir == t1, 1.0, 0.0)
    cot = cot_ref[...].astype(F32)
    c0 = (columns_of(weight_ref[0:1, :]) * cot).astype(BF16)
    c1 = (columns_of(weight_ref[1:2, :]) * cot).astype(BF16)
    rows = dot((p0 + p1).astype(BF16), mi_ref[...], 1, 0).astype(BF16)
    cots = (dot(p0.astype(BF16), c0, 1, 0) + dot(p1.astype(BF16), c1, 1, 0)).astype(BF16)
    S[:, 0] = rows.reshape(32, 16, 128)
    S[:, 1] = cots.reshape(32, 16, 128)

    pl.semaphore_wait(barrier, 46)

    send(S.at[partner], X.at[y, x, c], sA, rA.at[0], (partner, tp))
    for r in ORDER[1:]:
        d = (16 - r) % 16
        q = PLACE[r] * 2
        for core in range(2):
            dest = chip(d, core)
            send(S.at[dest], X.at[y, x, q + c], sA, rA.at[q // K], (dest, tp))
    X[y, x, c] = S[sp]

    lane = iota((32, 128), 1)

    def prepare():
        opt = jnp.transpose(jnp.pad(op_ref[...].astype(F32), ((0, 64), (0, 64))))
        OB[sp] = jnp.where(lane < 64, opt[0:32], pltpu.roll(opt[32:64], 64, 1)).astype(BF16)
        k0, k1 = columns_of(t0), columns_of(t1)
        for n in range(4):
            il = (iota((128, 128), 1) + 128 * n).astype(F32)
            PT[:, 128 * n : 128 * n + 128] = jnp.where((k0 == il) | (k1 == il), 1.0, 0.0).astype(BF16)

        TT[...] = jnp.zeros_like(TT)
        TT[0:31, 0:64] = taps_ref[...].astype(F32)
        TT[31:32, 0:64] = gain_ref[...]
        tt = jnp.transpose(TT[...])
        gain = jnp.broadcast_to(tt[0:64, 31:32], (64, 128))
        for o in range(31):
            TB[o] = jnp.broadcast_to(tt[0:64, o : o + 1], (64, 128))
        normed = (co_ref[...].astype(F32) - mean_ref[...]) * rstd_ref[...]
        scaled = normed * gain
        sig = jax.nn.sigmoid(scaled)
        NM[...] = normed
        FC[...] = sig * (1.0 + scaled * (1.0 - sig)) * gain
        MX[...] = (scaled * sig).astype(BF16)
        SB[...] = jnp.zeros_like(SB)

    def share_projection():
        send(OB.at[sp], OB.at[sp], sO, rO, (partner, tp))
        for d in range(1, 16):
            for core in range(2):
                send(OB.at[sp], OB.at[sp], sO, rO, (chip(d, core), tp))

    def q0(g, h):
        return g * K + h * HK

    def one(h, fo, lo, hi):
        yy, xx = (0, fo) if h == 0 else (fo, 0)
        return X.at[(y + yy) % 4, (x + xx) % 4, lo:hi]

    def line(h, so, lo, hi):
        return X.at[(y + so) % 4, :, lo:hi] if h == 0 else X.at[:, (x + so) % 4, lo:hi]

    def copy_to(ref, sem, dev):
        send(ref, ref, sB, sem, (sp, dev))

    def B0(g):
        first = 1 if g == 0 else 0
        wait(X.at[0, 0, g * K + first : g * K + K], rA.at[g])
        for h in range(2):
            q = q0(g, h)
            copy_to(one(h, 0, q, q + HK), b1.at[g, h, 0], J(h, 1, 0))
            copy_to(one(h, 0, q, q + HK), b1.at[g, h, 1], J(h, 3, 0))

    def B1(g):
        for h in range(2):
            q = q0(g, h)
            wait(one(h, 3, q, q + HK), b1.at[g, h, 0])
            copy_to(one(h, 3, q, q + QK), b1f.at[g, h, 0], J(h, 1, 0))
            wait(one(h, 1, q, q + HK), b1.at[g, h, 1])
            copy_to(one(h, 1, q + QK, q + HK), b1f.at[g, h, 1], J(h, 3, 0))

    def B2(g):
        for h in range(2):
            q = q0(g, h)
            wait(one(h, 2, q, q + QK), b1f.at[g, h, 0])
            wait(one(h, 2, q + QK, q + HK), b1f.at[g, h, 1])
            copy_to(line(h, 0, q, q + HK), b2.at[g, h, 0], J(h, 0, 1))
            copy_to(line(h, 0, q, q + HK), b2.at[g, h, 1], J(h, 0, 3))

    def B3(g):
        for h in range(2):
            q = q0(g, h)
            wait(line(h, 3, q, q + HK), b2.at[g, h, 0])
            copy_to(line(h, 3, q, q + QK), b2f.at[g, h, 0], J(h, 0, 1))
            wait(line(h, 1, q, q + HK), b2.at[g, h, 1])
            copy_to(line(h, 1, q + QK, q + HK), b2f.at[g, h, 1], J(h, 0, 3))

    def C(g):
        for h in range(2):
            q = q0(g, h)
            wait(line(h, 2, q, q + QK), b2f.at[g, h, 0])
            wait(line(h, 2, q + QK, q + HK), b2f.at[g, h, 1])
        if g == 0:
            for load in loads:
                load.wait()
        part = []
        for a in range(2):
            part.append(
                jnp.concatenate(
                    [X[j // 4, j % 4, g * K : g * K + K, a].reshape(RG, 128) for j in range(16)], axis=1
                )
            )
        both = dot(W[0:352], part[0], 1, 1)
        hg = dot(W[352:528], part[1], 1, 1)
        gate, up = both[0:176], both[176:352]
        gs = jax.nn.sigmoid(gate)
        act = gate * gs
        cols = slice(RG * g, RG * g + RG)
        gd = (hg * up * gs * (1.0 + gate * (1.0 - gs))).astype(BF16)
        ud = (hg * act).astype(BF16)
        DT[0:176, cols] = gd
        DT[176:352, cols] = ud
        DT[352:528, cols] = (act * up).astype(BF16)
        partial = dot(DT[0:352, cols], W[0:352], 0, 0)
        for j in range(16):
            yy, xx = j // 4, j % 4
            block = partial[:, 128 * j : 128 * j + 128].astype(BF16)
            PB[g, 0, xx, yy] = block[0:RH]
            PB[g, 1, yy, xx] = block[RH:RG]
        for h in range(2):
            f = (x, y)[h]
            far = (f + 2) % 4
            send(PB.at[g, h, far, 0:2], T1.at[g, h, 0], s1, r1.at[g, h, 0], (sp, J(h, 1, 0)))
            send(PB.at[g, h, far, 2:4], T1.at[g, h, 1], s1, r1.at[g, h, 1], (sp, J(h, 3, 0)))

    def R1(g):
        for h in range(2):
            f = (x, y)[h]
            nxt, prv = (f + 1) % 4, (f + 3) % 4
            wait(T1.at[g, h, 0], r1.at[g, h, 0])
            PB[g, h, nxt, 0:2] = (PB[g, h, nxt, 0:2].astype(F32) + T1[g, h, 0].astype(F32)).astype(BF16)
            send(PB.at[g, h, nxt], T2.at[g, h, 0], s1, r2.at[g, h, 0], (sp, J(h, 1, 0)))
            wait(T1.at[g, h, 1], r1.at[g, h, 1])
            PB[g, h, prv, 2:4] = (PB[g, h, prv, 2:4].astype(F32) + T1[g, h, 1].astype(F32)).astype(BF16)
            send(PB.at[g, h, prv], T2.at[g, h, 1], s1, r2.at[g, h, 1], (sp, J(h, 3, 0)))

    def R2(g):
        for h in range(2):
            f, s = ((x, y), (y, x))[h]
            wait(T2.at[g, h, 0], r2.at[g, h, 0])
            wait(T2.at[g, h, 1], r2.at[g, h, 1])
            Q[g, h] = (
                PB[g, h, f].astype(F32) + T2[g, h, 0].astype(F32) + T2[g, h, 1].astype(F32)
            ).astype(BF16)
            for d in range(1, 4):
                send(Q.at[g, h, (s + d) % 4], V.at[g, h, d - 1], s3, r3.at[g, h], (sp, J(h, 0, d)))

    def R3(g):
        for h in range(2):
            s = (y, x)[h]
            wait(V.at[g, h], r3.at[g, h])
            total = Q[g, h, s].astype(F32)
            for d in range(3):
                total = total + V[g, h, d].astype(F32)
            FN[g, h] = total.astype(BF16).reshape(HK, 16, 128)
            for k in range(HK):
                q = q0(g, h) + k
                r = ORDER[q // 2]
                if r == 0:
                    continue
                send(FN.at[g, h, k], RT.at[sp], sR, rR, (chip(r, q % 2), tp))
            if g == 0 and h == 0:
                send(FN.at[0, 0, 1 - c], RT.at[sp], sR, rR, (partner, tp))
                RT[sp] = FN[0, 0, c]

    def grads(lo, hi):
        def step(jp, carry):
            at = pl.ds(pl.multiple_of(jp * 256, 256), 256)
            rhs = jnp.concatenate(
                [X[jp // 2, 2 * (jp % 2) + i, :, 0].reshape(512, 128) for i in range(2)], axis=1
            )
            GO[0:352, at] = dot(DT[0:352], rhs, 1, 0).astype(BF16)
            rhs = jnp.concatenate(
                [X[jp // 2, 2 * (jp % 2) + i, :, 1].reshape(512, 128) for i in range(2)], axis=1
            )
            GO[352:528, at] = dot(DT[352:528], rhs, 1, 0).astype(BF16)
            return carry

        lax.fori_loop(lo, hi, step, 0)

    plan = {"B0": B0, "B1": B1, "B2": B2, "B3": B3, "C": C, "R1": R1, "R2": R2, "R3": R3}
    for t in range(STRIDE * (G - 1) + 1 + max(lag for _, lag in STEPS)):
        for name, lag in STEPS:
            g, off = (t - lag) // STRIDE, (t - lag) % STRIDE
            if off == 0 and 0 <= g < G:
                plan[name](g)
        if t == 0:
            prepare()
        if t == OUT_AT:
            share_projection()

    grads(0, 8)

    wait(OB.at[0:31], rO)
    for j in range(16):
        a, b = OB[2 * j].astype(F32), OB[2 * j + 1].astype(F32)
        OPT[j, 0:32] = jnp.where(lane < 64, a, pltpu.roll(b, 64, 1)).astype(BF16)
        OPT[j, 32:64] = jnp.where(lane < 64, pltpu.roll(a, 64, 1), b).astype(BF16)

    wait(RT.at[0:31], rR)
    mine = dot(PT[...], RT[...].reshape(512, 128), 1, 0)
    stream = (cot_ref[...].astype(F32) + mine).astype(BF16)
    FS[tp] = stream
    stream_out[...] = stream
    for o in PEERS:
        send(FS.at[tp], FS.at[tp], sF, rF.at[o], (sp, J(0, o % 4, o // 4)))
    acc = jnp.zeros((64, 128), F32)

    def pair_sum(o):
        k = J(0, -o % 4, -(o // 4) % 4)
        wait(GI.at[k], rD.at[o])
        GS[k] = (GP[c, k].astype(F32) + GI[k].astype(F32)).astype(BF16)

        @pl.when(k == z)
        def _():
            GR[z] = GS[z]

        @pl.when(k != z)
        def _():
            send(GS.at[k], GR.at[z], sG, rG, (2 * k + c, tp))

    pieces = (0,) + PEERS
    for n, o in enumerate(pieces):
        k = J(0, -o % 4, -(o // 4) % 4)
        if o:
            wait(FS.at[k], rF.at[o])
        piece = FS[k]
        gt = dot(MX[...], piece, 1, 0)
        top, bottom = gt[0:32], gt[32:64]
        GP[0, k] = jnp.where(lane < 64, top, pltpu.roll(bottom, 64, 1)).astype(BF16)
        GP[1, k] = jnp.where(lane < 64, pltpu.roll(top, 64, 1), bottom).astype(BF16)
        send(GP.at[1 - c, k], GI.at[k], sD, rD.at[o], (partner, tp))
        acc = acc + dot(OPT[k], piece, 1, 1)
        if n >= 4:
            pair_sum(pieces[n - 4])

    ng = acc * FC[...]
    normed = NM[...]
    SB[0:1, :] = jnp.sum(ng, axis=0, keepdims=True)
    SB[1:2, :] = jnp.sum(ng * normed, axis=0, keepdims=True)
    for o in range(1, 16):
        send(SB, SR.at[tp], sS, rS, (sp, J(0, o % 4, o // 4)))
    SR[tp] = SB[...]

    for o in pieces[12:]:
        pair_sum(o)

    wait(SR.at[0:15], rS)
    sums = jnp.sum(SR[...], axis=0) * (1.0 / 1024.0)
    cg = rstd_ref[...] * (ng - sums[0:1, :] - normed * sums[1:2, :])
    CG[...] = cg
    send(CG, HB, sH, rH, ((sp + 31) % 32, tp))
    wait(HB, rH)
    halo = jnp.where(sp == 31, 0.0, HB[...])
    lanes = iota((64, 128), 1)
    unit = TB[30] * cg
    for o in range(30):
        lead = 30 - o
        unit = unit + TB[o] * pltpu.roll(jnp.where(lanes >= lead, cg, halo), 128 - lead, 1)
    vs = jax.nn.sigmoid(vg_ref[...].astype(F32))
    value_out[...] = (unit * vs).astype(BF16)
    gating_out[...] = (unit * vv_ref[...].astype(F32) * vs * (1.0 - vs)).astype(BF16)

    wait(GR.at[0:15], rG)
    total = GR[0].astype(F32)
    for k in range(1, 16):
        total = total + GR[k].astype(F32)
    TT[0:32, :] = total
    TT[32:64, :] = pltpu.roll(total, 64, 1)
    proj_out[...] = jnp.transpose(TT[...])[0:64, 0:64]

    wait(S.at[0:31], sA)
    wait(OB.at[0:31], sO)
    wait(X.at[:, :, 0:30], sB)
    wait(PB.at[:, :, 0:3], s1)
    wait(Q.at[:, :, 0:3], s3)
    wait(RT.at[0:31], sR)
    wait(FS.at[0:15], sF)
    wait(GI, sD)
    wait(GR.at[0:15], sG)
    wait(SR.at[0:15], sS)
    wait(HB, sH)


def finish(
    go, proj, stream, value, gating,
    gate_out, up_out, down_out, proj_out, stream_out, value_out, gating_out, sems,
):
    pairs = [(go.at[176 * i : 176 * i + 176], r.at[0]) for i, r in enumerate((gate_out, up_out, down_out))]
    pairs += [(proj, proj_out), (stream, stream_out), (value, value_out), (gating, gating_out)]
    copies = [pltpu.make_async_copy(a, b, sems.at[i]) for i, (a, b) in enumerate(pairs)]
    for copy in copies:
        copy.start()
    for copy in copies:
        copy.wait()


def shards(
    moe_input, cotangent, routes, route_weight, w_gate, w_up, w_down, v_value, v_gate, conv_out,
    row_mean, row_rstd, ln_gain, taps, out_proj,
):
    vmem = pl.BlockSpec(memory_space=pltpu.VMEM)
    hbm = pl.BlockSpec(memory_space=pltpu.HBM)
    dma = pltpu.SemaphoreType.DMA
    v = pltpu.VMEM
    out = pl.pallas_call(
        kernel,
        out_shape=(
            v((528, 2048), BF16),
            v((64, 64), F32),
            v((128, 128), BF16),
            v((64, 128), BF16),
            v((64, 128), BF16),
        ),
        in_specs=[vmem] * 4 + [hbm] * 3 + [vmem] * 8,
        out_specs=(vmem,) * 5,
        scratch_shapes=[
            v((32, 2, 16, 128), BF16),
            v((4, 4, 32, 2, 16, 128), BF16),
            v((528, 2048), BF16),
            v((G, 2, 4, 4, RH, 128), BF16),
            v((G, 2, 2, 2, RH, 128), BF16),
            v((G, 2, 2, 4, RH, 128), BF16),
            v((G, 2, 4, RH, 128), BF16),
            v((G, 2, 3, RH, 128), BF16),
            v((G, 2, HK, 16, 128), BF16),
            v((32, 16, 128), BF16),
            v((16, 128, 128), BF16),
            v((528, 512), BF16),
            v((128, 512), BF16),
            v((32, 32, 128), BF16),
            v((16, 64, 128), BF16),
            v((128, 128), F32),
            v((31, 64, 128), F32),
            v((64, 128), F32),
            v((64, 128), F32),
            v((64, 128), BF16),
            v((2, 16, 32, 128), BF16),
            v((16, 32, 128), BF16),
            v((16, 32, 128), BF16),
            v((16, 32, 128), BF16),
            v((8, 128), F32),
            v((16, 8, 128), F32),
            v((64, 128), F32),
            v((64, 128), F32),
            dma((3,)),
            dma(()), dma((G,)),
            dma(()), dma((G, 2, 2)), dma((G, 2, 2)), dma((G, 2, 2)), dma((G, 2, 2)),
            dma(()), dma((G, 2, 2)), dma((G, 2, 2)), dma(()), dma((G, 2)),
            dma(()), dma(()), dma(()), dma((16,)),
            dma(()), dma(()), dma(()), dma((16,)), dma(()), dma(()),
            dma(()), dma(()), dma(()), dma(()),
        ],
        compiler_params=pltpu.CompilerParams(
            collective_id=0, has_side_effects=True, vmem_limit_bytes=56 * 1024 * 1024
        ),
    )(
        routes.T, route_weight.T, moe_input, cotangent, w_gate, w_up, w_down, v_value.T, v_gate.T,
        conv_out.T, row_mean.reshape(1, 128), row_rstd.reshape(1, 128), ln_gain.reshape(1, 64), taps,
        out_proj,
    )
    shapes = ((1, 176, 2048),) * 3 + ((64, 64), (128, 128), (64, 128), (64, 128))
    kinds = (BF16, BF16, BF16, F32, BF16, BF16, BF16)
    out = pl.pallas_call(
        finish,
        out_shape=tuple(jax.ShapeDtypeStruct(a, b) for a, b in zip(shapes, kinds)),
        in_specs=[vmem] * 5,
        out_specs=(hbm,) * 7,
        scratch_shapes=[dma((7,))],
        compiler_params=pltpu.CompilerParams(vmem_limit_bytes=4 * 1024 * 1024),
    )(*out)
    gate_g, up_g, down_g, proj_g, stream, value_t, gating_t = out
    return gate_g, up_g, down_g, proj_g, stream, value_t.T, gating_t.T


def solution(mesh):
    return jax.shard_map(
        shards,
        mesh=mesh,
        in_specs=(
            P("sp", "tp"),
            P("sp", "tp"),
            P("sp", None),
            P("sp", None),
            P("sp", "tp", None),
            P("sp", "tp", None),
            P("sp", "tp", None),
            P("sp", "tp"),
            P("sp", "tp"),
            P("sp", "tp"),
            P("sp"),
            P("sp"),
            P("tp"),
            P(None, "tp"),
            P("sp", "tp"),
        ),
        out_specs=(
            P("sp", "tp", None),
            P("sp", "tp", None),
            P("sp", "tp", None),
            P("sp", "tp"),
            P("sp", "tp"),
            P("sp", "tp"),
            P("sp", "tp"),
        ),
        check_vma=False,
    )
```
